32 devices in a mesh: sp: 16 (over z, y, x), tp: 2 (over core).
Axes of the slice: x: 2, y: 2, z: 4, core: 2. Of those that a mesh axis runs over, the one named last changes fastest.
Arguments:
- queries_small: bfloat16 [4096, 1024], P('sp', 'tp'), may hold values from -160 to 160
- queries_large: bfloat16 [4096, 1024], P('sp', 'tp'), may hold values from -160 to 160
- kv_small: bfloat16 [4096, 128], P('sp'), may hold values from -4 to 4
- kv_large: bfloat16 [4096, 256], P('sp'), may hold values from -4 to 4
- cum_small: float32 [16, 4096], P('tp', 'sp'), may hold values from -514 to 0, as said below
- cum_large: float32 [8, 4096], P('tp', 'sp'), may hold values from -514 to 0, as said below
- residual: bfloat16 [4096, 2048], P(('sp', 'tp')), may hold values from -6 to 6
- out_small: bfloat16 [1024, 2048], replicated, may hold values from -0.125 to 0.125
- out_large: bfloat16 [1024, 2048], replicated, may hold values from -0.125 to 0.125
- gain_mix: float32 [2048], replicated, may hold values from 0.1 to 1.9
- gain_route: float32 [2048], replicated, may hold values from 0.1 to 1.9
- gain_blend: float32 [2048], replicated, may hold values from 0.1 to 1.9
- w_gate: bfloat16 [32, 2048, 1024], P(('sp', 'tp')), may hold values from -0.125 to 0.125
- w_up: bfloat16 [32, 2048, 1024], P(('sp', 'tp')), may hold values from -0.125 to 0.125
- w_down: bfloat16 [32, 1024, 2048], P(('sp', 'tp')), may hold values from -0.1875 to 0.1875
- route: int32 [2, 4096], P(None, ('sp', 'tp')), may hold values from 0 to 31, as said below
- route_bias: float32 [4096], P(('sp', 'tp')), may hold values from -6 to 6
Outputs:
- result: bfloat16 [4096, 2048], P(('sp', 'tp'))
The draws below stay inside these ranges and needn't reach their ends.
Inputs may be any that keep to these rules, and one draw needn't show every extreme that they name: `cum_small`: each row is non-increasing along positions. `cum_large`: each row is non-increasing along positions. route[0, t] and route[1, t] are different experts of the same group of 8 consecutive experts. Among the 128 positions of one device (aligned blocks), no expert is named by more than 16 of them; in every draw all experts of one group are named by exactly 16 positions of every device. Within one device's positions the loads of the experts of one group differ by at most 2.
All inputs are finite; a program needn't handle non-finite values.
Results may differ from the reference program's by a relative error of at most 0.014.
Values may be sent and summed in bfloat16 or wider, within the bound.
A program may use at most 128 MiB of HBM per device.

```python
import math
import jax
import jax.numpy as jnp
from jax import lax

D = 2048
HA = 16
DA = 64
HB = 8
DB = 128
FF = 1024
GROUPS = 4
TOK_DEV = 256
SEQUENCE_TOKENS = 4096
ROWS_DEV = 128
EXPERTS = 32
EPG = 8
CAP = 16
N_SP = 16
N_TP = 2


def shared_keys(root_random_key, head_size):
    return jnp.clip(jax.random.normal(jax.random.fold_in(root_random_key, 5), (SEQUENCE_TOKENS, head_size), jnp.float32), -4.0, 4.0)


def key_value_rows(key, label, head_size):
    root_random_key = jax.random.fold_in(key, label)
    key_rows = shared_keys(root_random_key, head_size)
    value_rows = jnp.clip(jax.random.normal(jax.random.fold_in(root_random_key, 6), (SEQUENCE_TOKENS, head_size), jnp.float32), -4.0, 4.0)
    return jnp.concatenate([key_rows, value_rows], axis=1).astype(jnp.bfloat16)


def query_rows(key, label, head_count, head_size):
    root_random_key = jax.random.fold_in(key, label)
    drawn = jnp.clip(jax.random.normal(jax.random.fold_in(root_random_key, 9), (SEQUENCE_TOKENS, head_count * head_size), jnp.float32), -4.0, 4.0)
    return drawn.astype(jnp.bfloat16)


def gate_totals(key, label, head_count):
    root_random_key = jax.random.fold_in(key, label)
    order = jax.random.permutation(jax.random.fold_in(root_random_key, 1), head_count)
    slow_heads = order < head_count // 2
    slow_total = jnp.exp(jax.random.uniform(jax.random.fold_in(root_random_key, 3), (head_count,), jnp.float32, math.log(0.8), math.log(1.6)))
    fast_rate = jnp.exp(jax.random.uniform(jax.random.fold_in(root_random_key, 4), (head_count,), jnp.float32, math.log(0.01), math.log(1.0 / 30.0)))
    rates = jnp.where(slow_heads, slow_total / SEQUENCE_TOKENS, fast_rate)
    factors = jnp.exp(jax.random.uniform(jax.random.fold_in(root_random_key, 5), (SEQUENCE_TOKENS // TOK_DEV,), jnp.float32, math.log(0.5), math.log(2.0)))
    factors = jnp.repeat(factors, TOK_DEV)
    rough = jax.random.uniform(jax.random.fold_in(root_random_key, 6), (head_count, SEQUENCE_TOKENS), jnp.float32, 0.5, 1.5)
    gate_logarithms = -rates[:, None] * factors[None, :] * rough
    spike_position = jax.random.randint(jax.random.fold_in(root_random_key, 7), (3,), 0, SEQUENCE_TOKENS)
    spike_penalty = jax.random.uniform(jax.random.fold_in(root_random_key, 8), (3,), jnp.float32, 0.2, 0.4)
    spot_locations = jnp.arange(SEQUENCE_TOKENS, dtype=jnp.int32)
    spike_events = jnp.sum(jnp.where(spot_locations[None, :] == spike_position[:, None], jnp.log(1.0 - spike_penalty)[:, None], 0.0), axis=0)
    gate_logarithms = gate_logarithms + spike_events[None, :]
    return jnp.cumsum(gate_logarithms, axis=1).astype(jnp.float32)


def draw_queries_small(key, part):
    return query_rows(key, 11, HA, DA)


def draw_queries_large(key, part):
    return query_rows(key, 13, HB, DB)


def draw_kv_small(key, part):
    return key_value_rows(key, 11, DA)


def draw_kv_large(key, part):
    return key_value_rows(key, 13, DB)


def draw_cum_small(key, part):
    return gate_totals(key, 31, HA)


def draw_cum_large(key, part):
    return gate_totals(key, 33, HB)


def draw_route(key, part):
    block_count = SEQUENCE_TOKENS // ROWS_DEV
    full_group = jax.random.randint(jax.random.fold_in(key, 21), (), 0, GROUPS)

    def one_block(block_index):
        block_key = jax.random.fold_in(jax.random.fold_in(key, 22), block_index)
        order = jax.random.permutation(jax.random.fold_in(block_key, 1), ROWS_DEV)
        spot_locations = jnp.arange(ROWS_DEV, dtype=jnp.int32)
        others = jax.random.randint(jax.random.fold_in(block_key, 2), (ROWS_DEV,), 0, GROUPS - 1)
        group_at = jnp.where(spot_locations < ROWS_DEV // 2, full_group, (full_group + 1 + others) % GROUPS)
        marked = (group_at[:, None] == jnp.arange(GROUPS, dtype=jnp.int32)[None, :]).astype(jnp.int32)
        ranked = jnp.sum((jnp.cumsum(marked, axis=0) - 1) * marked, axis=1)
        shifts = jax.random.randint(jax.random.fold_in(block_key, 3), (GROUPS,), 0, EPG)
        offset = ranked + shifts[group_at]
        first_inner = offset % EPG
        second_inner = (offset + 1 + ranked // EPG % (EPG - 1)) % EPG
        chosen = jnp.stack([group_at * EPG + first_inner, group_at * EPG + second_inner]).astype(jnp.int32)
        return jnp.zeros((2, ROWS_DEV), jnp.int32).at[:, order].set(chosen)
    blocks = jax.vmap(one_block)(jnp.arange(block_count, dtype=jnp.int32))
    return blocks.transpose(1, 0, 2).reshape(2, SEQUENCE_TOKENS)


def block_scale(key, extent, split, low, largest):
    gain = 1.0
    for position, shards_of in split:
        steps = jax.random.uniform(jax.random.fold_in(jax.random.fold_in(key, 6), position), (shards_of,), jnp.float32, low / len(split), largest / len(split))
        gain = gain * jnp.repeat(jnp.exp(steps), extent[position] // shards_of).reshape((-1,) + (1,) * (len(extent) - 1 - position))
    return gain


def noise(rng, dims, deviation, limit, split=(), kind=jnp.bfloat16):
    array = jax.random.normal(rng, dims, jnp.float32) * deviation
    if len(split) > 0:
        array = block_scale(rng, dims, split, -0.22, 0.18) * array
    return jnp.clip(array, min=-limit, max=limit).astype(kind)


def setup_inputs(seed: int = 0) -> dict:
    streams_of = jax.random.split(jax.random.key(seed), 18)
    return {
        "queries_small": draw_queries_small(jax.random.fold_in(streams_of[17], 71), 0),
        "queries_large": draw_queries_large(jax.random.fold_in(streams_of[17], 71), 0),
        "kv_small": draw_kv_small(jax.random.fold_in(streams_of[17], 71), 0),
        "kv_large": draw_kv_large(jax.random.fold_in(streams_of[17], 71), 0),
        "cum_small": draw_cum_small(jax.random.fold_in(streams_of[17], 71), 0),
        "cum_large": draw_cum_large(jax.random.fold_in(streams_of[17], 71), 0),
        "residual": noise(streams_of[6], (SEQUENCE_TOKENS, D), 1.0, 6.0, ((0, 32),)),
        "out_small": noise(streams_of[7], (HA * DA, D), D ** -0.5, 0.125),
        "out_large": noise(streams_of[8], (HB * DB, D), D ** -0.5, 0.125),
        "gain_mix": jnp.clip(1.0 + 0.18 * jax.random.normal(streams_of[9], (D,), jnp.float32), 0.1, 1.9),
        "gain_route": jnp.clip(1.0 + 0.18 * jax.random.normal(streams_of[10], (D,), jnp.float32), 0.1, 1.9),
        "gain_blend": jnp.clip(1.0 + 0.18 * jax.random.normal(streams_of[11], (D,), jnp.float32), 0.1, 1.9),
        "w_gate": noise(streams_of[12], (EXPERTS, D, FF), D ** -0.5, 0.125, ((0, 32),)),
        "w_up": noise(streams_of[13], (EXPERTS, D, FF), D ** -0.5, 0.125, ((0, 32),)),
        "w_down": noise(streams_of[14], (EXPERTS, FF, D), FF ** -0.5, 0.1875, ((0, 32),)),
        "route": draw_route(jax.random.fold_in(streams_of[17], 71), 0),
        "route_bias": noise(streams_of[16], (SEQUENCE_TOKENS,), 1.5, 6.0, ((0, 32),), jnp.float32),
    }


norm_eps = 1e-06

def rms_scale(values, gain_row):
    return values * lax.rsqrt(lax.optimization_barrier(jnp.mean(values * values, axis=-1, keepdims=True)) + norm_eps) * gain_row.astype(jnp.float32)

def attend_group(queries, keys_values, cumulative, head_count, head_size):
    key_rows = keys_values[:, :head_size].astype(jnp.float32)
    value_rows = keys_values[:, head_size:].astype(jnp.float32)
    block_rows = min(256, SEQUENCE_TOKENS)
    block_count = SEQUENCE_TOKENS // block_rows
    query_blocks = queries.reshape(block_count, block_rows, head_count, head_size)
    cum_blocks = cumulative.reshape(head_count, block_count, block_rows).transpose(1, 0, 2)
    key_pos = jnp.arange(SEQUENCE_TOKENS, dtype=jnp.int32)

    def one_block(inputs):
        query_block, cum_block, block_index = inputs
        scores = jnp.einsum('qhd,kd->hqk', query_block.astype(jnp.float32), key_rows) * head_size ** (-0.5)
        scores = scores + cum_block[:, :, None] - cumulative[:, None, :]
        query_pos = block_index * block_rows + jnp.arange(block_rows, dtype=jnp.int32)
        allowed = key_pos[None, None, :] <= query_pos[None, :, None]
        scores = jnp.where(allowed, scores, -jnp.inf)
        row_max = lax.optimization_barrier(jnp.max(scores, axis=-1, keepdims=True))
        weights = jnp.where(allowed, jnp.exp(scores - row_max), 0.0)
        rounded = lax.optimization_barrier(weights.astype(jnp.bfloat16)).astype(jnp.float32)
        numerator = jnp.einsum('hqk,kd->qhd', rounded, value_rows)
        denominator = lax.optimization_barrier(jnp.sum(weights, axis=-1)).T
        return (numerator / denominator[:, :, None]).astype(jnp.bfloat16)
    outputs = lax.map(one_block, (query_blocks, cum_blocks, jnp.arange(block_count, dtype=jnp.int32)))
    return outputs.reshape(SEQUENCE_TOKENS, head_count * head_size)

def reference(queries_small, queries_large, kv_small, kv_large, cum_small, cum_large, residual, out_small, out_large, gain_mix, gain_route, gain_blend, w_gate, w_up, w_down, route, route_bias):
    attn_small = attend_group(queries_small, kv_small, cum_small, HA, DA)
    attn_large = attend_group(queries_large, kv_large, cum_large, HB, DB)
    mixer_out = jnp.dot(attn_small, out_small, preferred_element_type=jnp.float32) + jnp.dot(attn_large, out_large, preferred_element_type=jnp.float32)
    mixed = (residual.astype(jnp.float32) + rms_scale(mixer_out, gain_mix)).astype(jnp.bfloat16)
    routed = rms_scale(mixed.astype(jnp.float32), gain_route).astype(jnp.bfloat16)
    flat_ids = route.reshape(-1)
    most_rows = N_SP * N_TP * CAP

    def one_expert(carried, inputs):
        expert_id, gate_w, up_w, down_w = inputs
        matches = flat_ids == expert_id
        picked = jnp.nonzero(matches, size=most_rows, fill_value=0)[0].astype(jnp.int32)
        valid_rows = jnp.arange(most_rows, dtype=jnp.int32) < jnp.sum(matches.astype(jnp.int32))
        expert_rows = routed[picked % SEQUENCE_TOKENS]
        gate_pre = jnp.dot(expert_rows, gate_w, preferred_element_type=jnp.float32)
        up_pre = jnp.dot(expert_rows, up_w, preferred_element_type=jnp.float32)
        hidden = (jax.nn.silu(gate_pre) * up_pre).astype(jnp.bfloat16)
        expert_out = jnp.dot(hidden, down_w, preferred_element_type=jnp.float32).astype(jnp.bfloat16)
        masked = jnp.where(valid_rows[:, None], expert_out.astype(jnp.float32), 0.0)
        return (carried.at[picked].add(masked), None)
    outputs, _ = lax.scan(one_expert, jnp.zeros((2 * SEQUENCE_TOKENS, D), jnp.float32), (jnp.arange(EXPERTS, dtype=jnp.int32), w_gate, w_up, w_down))
    blended = jax.nn.sigmoid(route_bias)[:, None] * outputs[:SEQUENCE_TOKENS] + jax.nn.sigmoid(-route_bias)[:, None] * outputs[SEQUENCE_TOKENS:]
    return (mixed.astype(jnp.float32) + rms_scale(blended, gain_blend)).astype(jnp.bfloat16)
```

```python
import functools
import math

import jax
import jax.numpy as jnp
from jax import lax
from jax.experimental import pallas as pl
from jax.experimental.pallas import tpu as pltpu
from jax.sharding import PartitionSpec as P

norm_eps = 1e-06
far_score = -1e30
log2e = math.log2(math.e)
MESH = pl.DeviceIdType.MESH


def rms_scale(values, gain_row):
    return (
        values * lax.rsqrt(jnp.mean(values * values, axis=-1, keepdims=True) + norm_eps) * gain_row
    )


def mesh_shape(mesh):
    coords = [tuple(device.coords) for device in mesh.devices.reshape(-1)]
    return tuple(1 + max(c[axis] for c in coords) - min(c[axis] for c in coords) for axis in (2, 1, 0))


def gather_kernel(dims, kv_ref, cum_ref, kv_all, cum_all, send_kv, send_cum, send_core, recv_kv, recv_cum, recv_core, own_sem):
    depth, rows_y, rows_x = dims
    plane = rows_y * rows_x
    me = lax.axis_index("sp")
    core = lax.axis_index("tp")
    mine_z = me // plane
    mine_y = me % plane // rows_x
    mine_x = me % rows_x
    half = kv_ref.shape[0] // 2
    barrier = pltpu.get_barrier_semaphore()
    peers = 0
    for step in range(1, depth):
        target = (mine_z + step) % depth * plane + me % plane
        pl.semaphore_signal(barrier, inc=1, device_id=(target, core), device_id_type=MESH)
        peers += 1
    for step in range(1, rows_y):
        target = mine_z * plane + (mine_y + step) % rows_y * rows_x + mine_x
        pl.semaphore_signal(barrier, inc=1, device_id=(target, core), device_id_type=MESH)
        peers += 1
    for step in range(1, rows_x):
        target = mine_z * plane + mine_y * rows_x + (mine_x + step) % rows_x
        pl.semaphore_signal(barrier, inc=1, device_id=(target, core), device_id_type=MESH)
        peers += 1
    pl.semaphore_signal(barrier, inc=1, device_id=(me, 1 - core), device_id_type=MESH)
    own_kv = pltpu.make_async_copy(kv_ref, kv_all.at[me], own_sem.at[0])
    own_cum = pltpu.make_async_copy(cum_ref, cum_all.at[me], own_sem.at[1])
    own_kv.start()
    own_cum.start()
    own_kv.wait()
    own_cum.wait()
    pl.semaphore_wait(barrier, peers + 1)

    def copies(shard, target, slot):
        part = kv_all.at[shard, pl.ds(core * half, half)]
        return (
            pltpu.make_async_remote_copy(
                src_ref=part, dst_ref=part, send_sem=send_kv.at[slot], recv_sem=recv_kv.at[shard],
                device_id=(target, core), device_id_type=MESH),
            pltpu.make_async_remote_copy(
                src_ref=cum_all.at[shard], dst_ref=cum_all.at[shard], send_sem=send_cum.at[slot],
                recv_sem=recv_cum.at[shard], device_id=(target, core), device_id_type=MESH),
        )

    def across(shard):
        part = kv_all.at[shard, pl.ds(core * half, half)]
        return pltpu.make_async_remote_copy(
            src_ref=part, dst_ref=part, send_sem=send_core.at[shard], recv_sem=recv_core.at[shard],
            device_id=(me, 1 - core), device_id_type=MESH)

    def arrived(shard):
        for copy in copies(shard, me, 0):
            copy.wait_recv()

    def other_half(shard):
        part = kv_all.at[shard, pl.ds((1 - core) * half, half)]
        return pltpu.make_async_remote_copy(
            src_ref=part, dst_ref=part, send_sem=send_core.at[shard], recv_sem=recv_core.at[shard],
            device_id=(me, 1 - core), device_id_type=MESH)

    def route(first_axis):
        size_a, size_b = (rows_y, rows_x) if first_axis == "y" else (rows_x, rows_y)
        here_a, here_b = (mine_y, mine_x) if first_axis == "y" else (mine_x, mine_y)

        def index(z, a, b):
            return z * plane + (a * rows_x + b if first_axis == "y" else b * rows_x + a)

        sends = []
        slot = 0
        for step in range(1, depth):
            sends.append((mine_z + step < depth, index(mine_z, here_a, here_b), index(mine_z + step, here_a, here_b), slot))
            slot += 1

        def start(items):
            for _, shard, target, number in items:
                for copy in copies(shard, target, number):
                    copy.start()

        for item in sends:
            pl.when(item[0])(functools.partial(start, [item]))
        for behind in range(depth):
            z = mine_z - behind
            items = []
            shard = index(z, here_a, here_b)
            for step in range(1, size_a):
                items.append((z >= 0, shard, index(mine_z, (here_a + step) % size_a, here_b), slot))
                slot += 1
            for step in range(1, size_b):
                items.append((z >= 0, shard, index(mine_z, here_a, (here_b + step) % size_b), slot))
                slot += 1
            sends += items

            def forward(items=items, shard=shard, behind=behind):
                if behind:
                    arrived(shard)
                start(items)
                if behind:
                    across(shard).start()

            pl.when(z >= 0)(forward)
        for behind in range(depth):
            z = mine_z - behind
            for step_a in range(1, size_a):
                shard = index(z, (here_a + size_a - step_a) % size_a, here_b)
                items = []
                for step in range(1, size_b):
                    items.append((z >= 0, shard, index(mine_z, here_a, (here_b + step) % size_b), slot))
                    slot += 1
                sends += items

                def relay(items=items, shard=shard):
                    arrived(shard)
                    start(items)
                    across(shard).start()

                pl.when(z >= 0)(relay)
        for behind in range(depth):
            z = mine_z - behind
            for step_b in range(1, size_b):
                for step_a in range(size_a):
                    shard = index(z, (here_a + size_a - step_a) % size_a, (here_b + size_b - step_b) % size_b)

                    def last(shard=shard):
                        arrived(shard)
                        across(shard).start()

                    pl.when(z >= 0)(last)
        for behind in range(depth):
            z = mine_z - behind

            def settle(z=z):
                for place in range(plane):

                    def finish_half(shard=z * plane + place):
                        other_half(shard).wait_recv()
                        across(shard).wait_send()

                    pl.when(z * plane + place != me)(finish_half)

            pl.when(z >= 0)(settle)
        for item in sends:

            def sent(item=item):
                for copy in copies(item[1], item[2], item[3]):
                    copy.wait_send()

            pl.when(item[0])(sent)

    pl.when(core == 0)(functools.partial(route, "y"))
    pl.when(core == 1)(functools.partial(route, "x"))


def gather_keys(dims, kv, cum):
    shards = lax.axis_size("sp")
    depth, rows_y, rows_x = dims
    slots = depth - 1 + depth * (rows_y + rows_x - 2) + depth * (rows_y - 1) * (rows_x - 1)
    dma = pltpu.SemaphoreType.DMA
    return pl.pallas_call(
        functools.partial(gather_kernel, dims),
        out_shape=(
            jax.ShapeDtypeStruct((shards,) + kv.shape, kv.dtype),
            jax.ShapeDtypeStruct((shards,) + cum.shape, cum.dtype),
        ),
        in_specs=[pl.BlockSpec(memory_space=pltpu.VMEM)] * 2,
        out_specs=(pl.BlockSpec(memory_space=pltpu.VMEM),) * 2,
        scratch_shapes=[
            dma((slots,)), dma((slots,)), dma((shards,)), dma((shards,)), dma((shards,)), dma((shards,)), dma((2,)),
        ],
        compiler_params=pltpu.CompilerParams(collective_id=0, has_side_effects=True),
        name="gather_keys",
    )(kv, cum)


def attend_kernel(head_shape, group, q_small, q_large, kv_all, cum_all, o_small, o_large, qs, ql, top, total, acc_s, acc_l):
    heads_small, heads_large, size_small, size_large = head_shape
    me = lax.axis_index("sp")
    tokens = q_small.shape[0]
    width = group * tokens
    for h in range(heads_small):
        qs[h] = q_small[:, h * size_small:(h + 1) * size_small]
    for h in range(heads_large):
        ql[h] = q_large[:, h * size_large:(h + 1) * size_large]
    top[...] = jnp.full_like(top, far_score)
    total[...] = jnp.zeros_like(total)
    acc_s[...] = jnp.zeros_like(acc_s)
    acc_l[...] = jnp.zeros_like(acc_l)

    def block(number, masked):
        first = number * group

        def run(heads, base, q_ref, acc_ref, column, size):
            scale = size ** (-0.5) * log2e

            def one(h, _):
                keys = kv_all[pl.ds(first, group), :, column:column + size].reshape(width, size)
                values = kv_all[pl.ds(first, group), :, column + size:column + 2 * size].reshape(width, size)
                gates = jnp.concatenate(
                    [cum_all[first + j, pl.ds(base + h, 1), :] for j in range(group)], axis=1
                ) * log2e
                scores = lax.dot_general(
                    q_ref[h], keys, (((1,), (1,)), ((), ())), preferred_element_type=jnp.float32
                ) * scale - gates
                if masked:
                    key_pos = lax.broadcasted_iota(jnp.int32, (tokens, width), 1) + first * tokens
                    query_pos = lax.broadcasted_iota(jnp.int32, (tokens, width), 0) + me * tokens
                    scores = jnp.where(key_pos <= query_pos, scores, far_score)
                before = top[base + h]
                newest = jnp.maximum(before, jnp.max(scores, axis=-1, keepdims=True))
                factor = jnp.exp2(before - newest)
                weights = jnp.exp2(scores - newest[:, :1])
                partial_sum = weights[:, :128]
                for j in range(1, width // 128):
                    partial_sum = partial_sum + weights[:, j * 128:(j + 1) * 128]
                top[base + h] = newest
                total[base + h] = total[base + h] * factor + partial_sum
                acc_ref[h] = acc_ref[h] * factor[:, :size] + jnp.dot(
                    weights.astype(jnp.bfloat16), values, preferred_element_type=jnp.float32
                )
                return 0

            lax.fori_loop(0, heads, one, 0)

        run(heads_small, 0, qs, acc_s, 0, size_small)
        run(heads_large, heads_small, ql, acc_l, 2 * size_small, size_large)

    last = me // group

    def whole(number, _):
        block(number, False)
        return 0

    lax.fori_loop(0, last, whole, 0)
    block(last, True)
    for h in range(heads_small):
        o_small[:, h * size_small:(h + 1) * size_small] = (
            acc_s[h] / jnp.sum(total[h], axis=-1, keepdims=True)
        ).astype(o_small.dtype)
    for h in range(heads_large):
        o_large[:, h * size_large:(h + 1) * size_large] = (
            acc_l[h] / jnp.sum(total[heads_small + h], axis=-1, keepdims=True)
        ).astype(o_large.dtype)


def attend(queries_small, queries_large, kv_all, cum_all, head_shape, group):
    heads_small, heads_large, size_small, size_large = head_shape
    tokens = queries_small.shape[0]
    heads = heads_small + heads_large
    return pl.pallas_call(
        functools.partial(attend_kernel, head_shape, group),
        out_shape=(
            jax.ShapeDtypeStruct(queries_small.shape, jnp.bfloat16),
            jax.ShapeDtypeStruct(queries_large.shape, jnp.bfloat16),
        ),
        in_specs=[pl.BlockSpec(memory_space=pltpu.VMEM)] * 4,
        out_specs=(pl.BlockSpec(memory_space=pltpu.VMEM),) * 2,
        scratch_shapes=[
            pltpu.VMEM((heads_small, tokens, size_small), jnp.bfloat16),
            pltpu.VMEM((heads_large, tokens, size_large), jnp.bfloat16),
            pltpu.VMEM((heads, tokens, 128), jnp.float32),
            pltpu.VMEM((heads, tokens, 128), jnp.float32),
            pltpu.VMEM((heads_small, tokens, size_small), jnp.float32),
            pltpu.VMEM((heads_large, tokens, size_large), jnp.float32),
        ],
        compiler_params=pltpu.CompilerParams(vmem_limit_bytes=56 * 1024 * 1024),
        name="attend",
    )(queries_small, queries_large, kv_all, cum_all)


def on_device(
    dims,
    queries_small,
    queries_large,
    kv_small,
    kv_large,
    cum_small,
    cum_large,
    residual,
    out_small,
    out_large,
    gain_mix,
    gain_route,
    gain_blend,
    w_gate,
    w_up,
    w_down,
    route,
    route_bias,
):
    tokens_here = queries_small.shape[0]
    heads_small = cum_small.shape[0]
    heads_large = cum_large.shape[0]
    size_small = kv_small.shape[1] // 2
    size_large = kv_large.shape[1] // 2
    kv_all, cum_all = gather_keys(
        dims,
        jnp.concatenate([kv_small, kv_large], axis=1),
        jnp.concatenate([cum_small, cum_large], axis=0),
    )
    group = math.gcd(dims[1] * dims[2], 4)
    attn_small, attn_large = attend(
        queries_small,
        queries_large,
        kv_all,
        cum_all,
        (heads_small, heads_large, size_small, size_large),
        group,
    )
    row_count = tokens_here // lax.axis_size("tp")
    whole_small, whole_large = (
        lax.all_to_all(attn_small, "tp", split_axis=0, concat_axis=1, tiled=True),
        lax.all_to_all(attn_large, "tp", split_axis=0, concat_axis=1, tiled=True),
    )
    mixer_out = jnp.dot(whole_small, out_small, preferred_element_type=jnp.float32) + jnp.dot(
        whole_large, out_large, preferred_element_type=jnp.float32
    )
    mixed = (residual.astype(jnp.float32) + rms_scale(mixer_out, gain_mix)).astype(jnp.bfloat16)
    routed = rms_scale(mixed.astype(jnp.float32), gain_route).astype(jnp.bfloat16)
    experts = lax.axis_size(("sp", "tp"))
    capacity = 4 * row_count // experts
    flat_ids = route.reshape(2 * row_count)
    marked = (flat_ids[:, None] == jnp.arange(experts, dtype=jnp.int32)[None, :]).astype(jnp.int32)
    ranked = jnp.sum((jnp.cumsum(marked, axis=0) - 1) * marked, axis=1)
    slot_ids = flat_ids * capacity + ranked
    dispatch_table = (
        slot_ids[:, None] == jnp.arange(experts * capacity, dtype=jnp.int32)[None, :]
    ).astype(jnp.bfloat16)
    dispatch_table = dispatch_table[:row_count] + dispatch_table[row_count:]
    outgoing = jnp.einsum(
        "rs,rd->sd", dispatch_table, routed, preferred_element_type=jnp.float32
    ).astype(jnp.bfloat16)
    outgoing = outgoing.reshape(experts, capacity, routed.shape[1])
    received = lax.all_to_all(outgoing, ("sp", "tp"), split_axis=0, concat_axis=0, tiled=True)
    row_total = received.shape[0] * received.shape[1]
    expert_rows = received.reshape(row_total, received.shape[2])
    gate_pre = jnp.dot(expert_rows, w_gate[0], preferred_element_type=jnp.float32)
    up_pre = jnp.dot(expert_rows, w_up[0], preferred_element_type=jnp.float32)
    hidden = (jax.nn.silu(gate_pre) * up_pre).astype(jnp.bfloat16)
    expert_out = jnp.dot(hidden, w_down[0], preferred_element_type=jnp.float32).astype(jnp.bfloat16)
    returned = lax.all_to_all(
        expert_out.reshape(received.shape), ("sp", "tp"), split_axis=0, concat_axis=0, tiled=True
    )
    picked = returned.reshape(experts * capacity, routed.shape[1])[slot_ids].astype(jnp.float32)
    blended = (
        jax.nn.sigmoid(route_bias)[:, None] * picked[:row_count]
        + jax.nn.sigmoid(-route_bias)[:, None] * picked[row_count:]
    )
    return (mixed.astype(jnp.float32) + rms_scale(blended, gain_blend)).astype(jnp.bfloat16)


def solution(mesh):
    in_specs = (
        P("sp", "tp"),
        P("sp", "tp"),
        P("sp", None),
        P("sp", None),
        P("tp", "sp"),
        P("tp", "sp"),
        P(("sp", "tp"), None),
        P(),
        P(),
        P(),
        P(),
        P(),
        P(("sp", "tp"), None, None),
        P(("sp", "tp"), None, None),
        P(("sp", "tp"), None, None),
        P(None, ("sp", "tp")),
        P(("sp", "tp")),
    )
    out_specs = P(("sp", "tp"), None)
    return jax.shard_map(
        functools.partial(on_device, mesh_shape(mesh)), mesh=mesh, in_specs=in_specs, out_specs=out_specs, check_vma=False
    )
```

```python
import functools
import math

import jax
import jax.numpy as jnp
from jax import lax
from jax.experimental import pallas as pl
from jax.experimental.pallas import tpu as pltpu
from jax.sharding import PartitionSpec as P

norm_eps = 1e-06
far_score = -1e30
log2e = math.log2(math.e)
MESH = pl.DeviceIdType.MESH


def rms_scale(values, gain_row):
    return (
        values * lax.rsqrt(jnp.mean(values * values, axis=-1, keepdims=True) + norm_eps) * gain_row
    )


def mesh_shape(mesh):
    coords = [tuple(device.coords) for device in mesh.devices.reshape(-1)]
    return tuple(1 + max(c[axis] for c in coords) - min(c[axis] for c in coords) for axis in (2, 1, 0))


def gather_kernel(dims, kv_ref, cum_ref, kv_all, cum_all, send_kv, send_cum, send_core, recv_kv, recv_cum, recv_core, own_sem):
    depth, rows_y, rows_x = dims
    plane = rows_y * rows_x
    me = lax.axis_index("sp")
    core = lax.axis_index("tp")
    mine_z = me // plane
    mine_y = me % plane // rows_x
    mine_x = me % rows_x
    half = kv_ref.shape[0] // 2
    barrier = pltpu.get_barrier_semaphore()
    peers = 0
    for step in range(1, depth):
        target = (mine_z + step) % depth * plane + me % plane
        pl.semaphore_signal(barrier, inc=1, device_id=(target, core), device_id_type=MESH)
        peers += 1
    for step in range(1, rows_y):
        target = mine_z * plane + (mine_y + step) % rows_y * rows_x + mine_x
        pl.semaphore_signal(barrier, inc=1, device_id=(target, core), device_id_type=MESH)
        peers += 1
    for step in range(1, rows_x):
        target = mine_z * plane + mine_y * rows_x + (mine_x + step) % rows_x
        pl.semaphore_signal(barrier, inc=1, device_id=(target, core), device_id_type=MESH)
        peers += 1
    pl.semaphore_signal(barrier, inc=1, device_id=(me, 1 - core), device_id_type=MESH)
    own_kv = pltpu.make_async_copy(kv_ref, kv_all.at[me], own_sem.at[0])
    own_cum = pltpu.make_async_copy(cum_ref, cum_all.at[me], own_sem.at[1])
    own_kv.start()
    own_cum.start()
    own_kv.wait()
    own_cum.wait()
    pl.semaphore_wait(barrier, peers + 1)

    def copies(shard, target, slot):
        part = kv_all.at[shard, pl.ds(core * half, half)]
        return (
            pltpu.make_async_remote_copy(
                src_ref=part, dst_ref=part, send_sem=send_kv.at[slot], recv_sem=recv_kv.at[shard],
                device_id=(target, core), device_id_type=MESH),
            pltpu.make_async_remote_copy(
                src_ref=cum_all.at[shard], dst_ref=cum_all.at[shard], send_sem=send_cum.at[slot],
                recv_sem=recv_cum.at[shard], device_id=(target, core), device_id_type=MESH),
        )

    def across(shard):
        part = kv_all.at[shard, pl.ds(core * half, half)]
        return pltpu.make_async_remote_copy(
            src_ref=part, dst_ref=part, send_sem=send_core.at[shard], recv_sem=recv_core.at[shard],
            device_id=(me, 1 - core), device_id_type=MESH)

    def arrived(shard):
        for copy in copies(shard, me, 0):
            copy.wait_recv()

    def other_half(shard):
        part = kv_all.at[shard, pl.ds((1 - core) * half, half)]
        return pltpu.make_async_remote_copy(
            src_ref=part, dst_ref=part, send_sem=send_core.at[shard], recv_sem=recv_core.at[shard],
            device_id=(me, 1 - core), device_id_type=MESH)

    def route(first_axis):
        size_a, size_b = (rows_y, rows_x) if first_axis == "y" else (rows_x, rows_y)
        here_a, here_b = (mine_y, mine_x) if first_axis == "y" else (mine_x, mine_y)

        def index(z, a, b):
            return z * plane + (a * rows_x + b if first_axis == "y" else b * rows_x + a)

        sends = []
        slot = 0
        for step in range(1, depth):
            sends.append((mine_z + step < depth, index(mine_z, here_a, here_b), index(mine_z + step, here_a, here_b), slot))
            slot += 1

        def start(items):
            for _, shard, target, number in items:
                for copy in copies(shard, target, number):
                    copy.start()

        for item in sends:
            pl.when(item[0])(functools.partial(start, [item]))
        for behind in range(depth):
            z = mine_z - behind
            items = []
            shard = index(z, here_a, here_b)
            for step in range(1, size_a):
                items.append((z >= 0, shard, index(mine_z, (here_a + step) % size_a, here_b), slot))
                slot += 1
            for step in range(1, size_b):
                items.append((z >= 0, shard, index(mine_z, here_a, (here_b + step) % size_b), slot))
                slot += 1
            sends += items

            def forward(items=items, shard=shard, behind=behind):
                if behind:
                    arrived(shard)
                start(items)
                if behind:
                    across(shard).start()

            pl.when(z >= 0)(forward)
        for behind in range(depth):
            z = mine_z - behind
            for step_a in range(1, size_a):
                shard = index(z, (here_a + size_a - step_a) % size_a, here_b)
                items = []
                for step in range(1, size_b):
                    items.append((z >= 0, shard, index(mine_z, here_a, (here_b + step) % size_b), slot))
                    slot += 1
                sends += items

                def relay(items=items, shard=shard):
                    arrived(shard)
                    start(items)
                    across(shard).start()

                pl.when(z >= 0)(relay)
        for behind in range(depth):
            z = mine_z - behind
            for step_b in range(1, size_b):
                for step_a in range(size_a):
                    shard = index(z, (here_a + size_a - step_a) % size_a, (here_b + size_b - step_b) % size_b)

                    def last(shard=shard):
                        arrived(shard)
                        across(shard).start()

                    pl.when(z >= 0)(last)
        for behind in range(depth):
            z = mine_z - behind

            def settle(z=z):
                for place in range(plane):

                    def finish_half(shard=z * plane + place):
                        other_half(shard).wait_recv()
                        across(shard).wait_send()

                    pl.when(z * plane + place != me)(finish_half)

            pl.when(z >= 0)(settle)
        for item in sends:

            def sent(item=item):
                for copy in copies(item[1], item[2], item[3]):
                    copy.wait_send()

            pl.when(item[0])(sent)

    pl.when(core == 0)(functools.partial(route, "y"))
    pl.when(core == 1)(functools.partial(route, "x"))


def gather_keys(dims, kv, cum):
    shards = lax.axis_size("sp")
    depth, rows_y, rows_x = dims
    slots = depth - 1 + depth * (rows_y + rows_x - 2) + depth * (rows_y - 1) * (rows_x - 1)
    dma = pltpu.SemaphoreType.DMA
    return pl.pallas_call(
        functools.partial(gather_kernel, dims),
        out_shape=(
            jax.ShapeDtypeStruct((shards,) + kv.shape, kv.dtype),
            jax.ShapeDtypeStruct((shards,) + cum.shape, cum.dtype),
        ),
        in_specs=[pl.BlockSpec(memory_space=pltpu.VMEM)] * 2,
        out_specs=(pl.BlockSpec(memory_space=pltpu.VMEM),) * 2,
        scratch_shapes=[
            dma((slots,)), dma((slots,)), dma((shards,)), dma((shards,)), dma((shards,)), dma((shards,)), dma((2,)),
        ],
        compiler_params=pltpu.CompilerParams(collective_id=0, has_side_effects=True),
        name="gather_keys",
    )(kv, cum)


def attend_kernel(head_shape, group, q_small, q_large, kv_all, cum_all, o_small, o_large, qs, ql, top, total, acc_s, acc_l):
    heads_small, heads_large, size_small, size_large = head_shape
    me = lax.axis_index("sp")
    tokens = q_small.shape[0]
    width = group * tokens
    for h in range(heads_small):
        qs[h] = q_small[:, h * size_small:(h + 1) * size_small]
    for h in range(heads_large):
        ql[h] = q_large[:, h * size_large:(h + 1) * size_large]
    top[...] = jnp.full_like(top, far_score)
    total[...] = jnp.zeros_like(total)
    acc_s[...] = jnp.zeros_like(acc_s)
    acc_l[...] = jnp.zeros_like(acc_l)

    def block(number, masked):
        first = number * group

        def run(heads, base, q_ref, acc_ref, column, size):
            scale = size ** (-0.5) * log2e

            def one(h, _):
                keys = kv_all[pl.ds(first, group), :, column:column + size].reshape(width, size)
                values = kv_all[pl.ds(first, group), :, column + size:column + 2 * size].reshape(width, size)
                gates = jnp.concatenate(
                    [cum_all[first + j, pl.ds(base + h, 1), :] for j in range(group)], axis=1
                ) * log2e
                scores = lax.dot_general(
                    q_ref[h], keys, (((1,), (1,)), ((), ())), preferred_element_type=jnp.float32
                ) * scale - gates
                if masked:
                    key_pos = lax.broadcasted_iota(jnp.int32, (tokens, width), 1) + first * tokens
                    query_pos = lax.broadcasted_iota(jnp.int32, (tokens, width), 0) + me * tokens
                    scores = jnp.where(key_pos <= query_pos, scores, far_score)
                before = top[base + h]
                newest = jnp.maximum(before, jnp.max(scores, axis=-1, keepdims=True))
                factor = jnp.exp2(before - newest)
                weights = jnp.exp2(scores - newest[:, :1])
                partial_sum = weights[:, :128]
                for j in range(1, width // 128):
                    partial_sum = partial_sum + weights[:, j * 128:(j + 1) * 128]
                top[base + h] = newest
                total[base + h] = total[base + h] * factor + partial_sum
                acc_ref[h] = acc_ref[h] * factor[:, :size] + jnp.dot(
                    weights.astype(jnp.bfloat16), values, preferred_element_type=jnp.float32
                )
                return 0

            lax.fori_loop(0, heads, one, 0)

        run(heads_small, 0, qs, acc_s, 0, size_small)
        run(heads_large, heads_small, ql, acc_l, 2 * size_small, size_large)

    last = me // group

    def whole(number, _):
        block(number, False)
        return 0

    lax.fori_loop(0, last, whole, 0)
    block(last, True)
    for h in range(heads_small):
        o_small[:, h * size_small:(h + 1) * size_small] = (
            acc_s[h] / jnp.sum(total[h], axis=-1, keepdims=True)
        ).astype(o_small.dtype)
    for h in range(heads_large):
        o_large[:, h * size_large:(h + 1) * size_large] = (
            acc_l[h] / jnp.sum(total[heads_small + h], axis=-1, keepdims=True)
        ).astype(o_large.dtype)


def attend(queries_small, queries_large, kv_all, cum_all, head_shape, group):
    heads_small, heads_large, size_small, size_large = head_shape
    tokens = queries_small.shape[0]
    heads = heads_small + heads_large
    return pl.pallas_call(
        functools.partial(attend_kernel, head_shape, group),
        out_shape=(
            jax.ShapeDtypeStruct(queries_small.shape, jnp.bfloat16),
            jax.ShapeDtypeStruct(queries_large.shape, jnp.bfloat16),
        ),
        in_specs=[pl.BlockSpec(memory_space=pltpu.VMEM)] * 4,
        out_specs=(pl.BlockSpec(memory_space=pltpu.VMEM),) * 2,
        scratch_shapes=[
            pltpu.VMEM((heads_small, tokens, size_small), jnp.bfloat16),
            pltpu.VMEM((heads_large, tokens, size_large), jnp.bfloat16),
            pltpu.VMEM((heads, tokens, 128), jnp.float32),
            pltpu.VMEM((heads, tokens, 128), jnp.float32),
            pltpu.VMEM((heads_small, tokens, size_small), jnp.float32),
            pltpu.VMEM((heads_large, tokens, size_large), jnp.float32),
        ],
        compiler_params=pltpu.CompilerParams(vmem_limit_bytes=56 * 1024 * 1024),
        name="attend",
    )(queries_small, queries_large, kv_all, cum_all)


def greet(depth, plane, cores, me, core):
    barrier = pltpu.get_barrier_semaphore()
    lanes = plane * cores
    here = me % plane * cores + core
    for step in range(1, depth):
        target = (me // plane + step) % depth * plane + me % plane
        pl.semaphore_signal(barrier, inc=1, device_id=(target, core), device_id_type=MESH)
    for step in range(1, lanes):
        other = (here + step) % lanes
        target = me // plane * plane + other // cores
        pl.semaphore_signal(barrier, inc=1, device_id=(target, other % cores), device_id_type=MESH)
    pl.semaphore_wait(barrier, depth - 1 + lanes - 1)


def distances(depth):
    found = [0]
    for step in range(1, depth):
        found += [step, -step]
    return found


def dispatch_kernel(depth, cores, rows_ref, meta_ref, received, metas, in_rows, stage, send_rows, send_meta, recv_rows, recv_meta, send_block, recv_block, own_sem):
    me = lax.axis_index("sp")
    core = lax.axis_index("tp")
    _, lanes, capacity, columns = stage.shape
    plane = lanes // cores
    slots = rows_ref.shape[1]
    mine = me // plane
    here = me % plane * cores + core
    own_rows = pltpu.make_async_copy(rows_ref.at[mine], in_rows.at[mine], own_sem.at[0, 0])
    own_meta = pltpu.make_async_copy(meta_ref.at[mine], metas.at[mine], own_sem.at[0, 1])
    own_rows.start()
    own_meta.start()
    greet(depth, plane, cores, me, core)

    def along(other):
        target = (other * plane + me % plane, core)
        return (
            pltpu.make_async_remote_copy(
                src_ref=rows_ref.at[other], dst_ref=in_rows.at[mine], send_sem=send_rows.at[other],
                recv_sem=recv_rows.at[mine], device_id=target, device_id_type=MESH),
            pltpu.make_async_remote_copy(
                src_ref=meta_ref.at[other], dst_ref=metas.at[mine], send_sem=send_meta.at[other],
                recv_sem=recv_meta.at[mine], device_id=target, device_id_type=MESH),
        )

    def incoming(other):
        target = (other * plane + me % plane, core)
        return (
            pltpu.make_async_remote_copy(
                src_ref=rows_ref.at[other], dst_ref=in_rows.at[other], send_sem=send_rows.at[other],
                recv_sem=recv_rows.at[other], device_id=target, device_id_type=MESH),
            pltpu.make_async_remote_copy(
                src_ref=meta_ref.at[other], dst_ref=metas.at[other], send_sem=send_meta.at[other],
                recv_sem=recv_meta.at[other], device_id=target, device_id_type=MESH),
        )

    def block(source, other, slot_of):
        return pltpu.make_async_remote_copy(
            src_ref=stage.at[source, other], dst_ref=received.at[source * lanes + slot_of],
            send_sem=send_block.at[source, other], recv_sem=recv_block.at[source, slot_of],
            device_id=(mine * plane + other // cores, other % cores), device_id_type=MESH)

    def keep(source):
        return pltpu.make_async_copy(
            stage.at[source, here], received.at[source * lanes + here], own_sem.at[1, source])

    steps = distances(depth)
    for step in steps[1:]:
        other = mine + step

        def launch(other=other):
            for copy in along(other):
                copy.start()

        pl.when((other >= 0) & (other < depth))(launch)
    own_rows.wait()
    own_meta.wait()
    for step in steps:
        other = mine + step

        def expand(other=other, step=step):
            if step:
                for copy in incoming(other):
                    copy.wait_recv()
            wanted = lax.broadcasted_iota(jnp.int32, (lanes * capacity, slots), 0).astype(jnp.float32) + 1.0
            first = metas[other, 0:1, :slots]
            second = metas[other, 1:2, :slots]
            table = jnp.where((wanted == first) | (wanted == second), 1.0, 0.0).astype(jnp.bfloat16)
            spread = jnp.dot(table, in_rows[other], preferred_element_type=jnp.float32)
            for lane in range(lanes):
                stage[other, lane] = spread[lane * capacity:(lane + 1) * capacity].astype(jnp.bfloat16)
            for move in range(1, lanes):
                block(other, (here + move) % lanes, here).start()
            keep(other).start()

        pl.when((other >= 0) & (other < depth))(expand)
    for source in range(depth):
        keep(source).wait()
        for move in range(1, lanes):
            block(source, (here + move) % lanes, (here + move) % lanes).wait_recv()
            block(source, (here + move) % lanes, here).wait_send()
    for step in steps[1:]:
        other = mine + step

        def sent(other=other):
            for copy in along(other):
                copy.wait_send()

        pl.when((other >= 0) & (other < depth))(sent)


def dispatch(rows, meta, lanes, cores, capacity):
    depth, slots, columns = rows.shape
    dma = pltpu.SemaphoreType.DMA
    vmem = pl.BlockSpec(memory_space=pltpu.VMEM)
    return pl.pallas_call(
        functools.partial(dispatch_kernel, depth, cores),
        out_shape=(
            jax.ShapeDtypeStruct((depth * lanes, capacity, columns), rows.dtype),
            jax.ShapeDtypeStruct(meta.shape, meta.dtype),
        ),
        in_specs=[vmem] * 2,
        out_specs=(vmem,) * 2,
        scratch_shapes=[
            pltpu.VMEM(rows.shape, rows.dtype),
            pltpu.VMEM((depth, lanes, capacity, columns), rows.dtype),
            dma((depth,)), dma((depth,)), dma((depth,)), dma((depth,)),
            dma((depth, lanes)), dma((depth, lanes)), dma((2, max(depth, 2))),
        ],
        compiler_params=pltpu.CompilerParams(
            collective_id=1, has_side_effects=True, vmem_limit_bytes=48 * 1024 * 1024),
        name="dispatch_rows",
    )(rows, meta)


def return_kernel(depth, cores, outs, metas, final, back, stage, send_block, recv_block, send_rows, recv_rows, own_sem):
    me = lax.axis_index("sp")
    core = lax.axis_index("tp")
    _, lanes, capacity, columns = back.shape
    plane = lanes // cores
    slots = final.shape[1]
    mine = me // plane
    here = me % plane * cores + core
    greet(depth, plane, cores, me, core)

    def block(source, other, slot_of):
        return pltpu.make_async_remote_copy(
            src_ref=outs.at[source * lanes + other], dst_ref=back.at[source, slot_of],
            send_sem=send_block.at[source, other], recv_sem=recv_block.at[source, slot_of],
            device_id=(mine * plane + other // cores, other % cores), device_id_type=MESH)

    def keep(source):
        return pltpu.make_async_copy(
            outs.at[source * lanes + here], back.at[source, here], own_sem.at[source])

    def along(other, slot_of):
        return pltpu.make_async_remote_copy(
            src_ref=stage.at[other], dst_ref=final.at[slot_of], send_sem=send_rows.at[other],
            recv_sem=recv_rows.at[slot_of], device_id=(other * plane + me % plane, core), device_id_type=MESH)

    steps = distances(depth)[::-1]
    for step in steps:
        other = mine + step

        def launch(other=other):
            for move in range(1, lanes):
                block(other, (here + move) % lanes, here).start()
            keep(other).start()

        pl.when((other >= 0) & (other < depth))(launch)
    for step in steps:
        other = mine + step

        def combine(other=other, step=step):
            keep(other).wait()
            for move in range(1, lanes):
                block(other, (here + move) % lanes, (here + move) % lanes).wait_recv()
            count = lanes * capacity
            width = metas.shape[2]
            wanted = lax.broadcasted_iota(jnp.int32, (count, width), 0).astype(jnp.float32) + 1.0
            weights = jnp.where(wanted == metas[other, 0:1, :], metas[other, 2:3, :], 0.0)
            weights = weights + jnp.where(wanted == metas[other, 1:2, :], metas[other, 3:4, :], 0.0)
            weights = weights.T[:slots]
            high = weights.astype(jnp.bfloat16)
            low = (weights - high.astype(jnp.float32)).astype(jnp.bfloat16)
            if capacity % 16:
                picked = jnp.concatenate(
                    [back[other, lane].astype(jnp.float32) for lane in range(lanes)], axis=0
                ).astype(jnp.bfloat16)
            else:
                picked = back[other].reshape(count, columns)
            mixed = jnp.dot(high, picked, preferred_element_type=jnp.float32) + jnp.dot(
                low, picked, preferred_element_type=jnp.float32)
            if step:
                stage[other] = mixed.astype(stage.dtype)
                along(other, mine).start()
            else:
                final[other] = mixed.astype(final.dtype)

        pl.when((other >= 0) & (other < depth))(combine)
    for step in steps:
        other = mine + step

        def settle(other=other, step=step):
            for move in range(1, lanes):
                block(other, (here + move) % lanes, here).wait_send()
            if step:
                along(other, other).wait_recv()
                along(other, mine).wait_send()

        pl.when((other >= 0) & (other < depth))(settle)


def give_back(outs, metas, lanes, cores, slots):
    depth = metas.shape[0]
    _, capacity, columns = outs.shape
    dma = pltpu.SemaphoreType.DMA
    vmem = pl.BlockSpec(memory_space=pltpu.VMEM)
    return pl.pallas_call(
        functools.partial(return_kernel, depth, cores),
        out_shape=jax.ShapeDtypeStruct((depth, slots, columns), outs.dtype),
        in_specs=[vmem] * 2,
        out_specs=vmem,
        scratch_shapes=[
            pltpu.VMEM((depth, lanes, capacity, columns), outs.dtype),
            pltpu.VMEM((depth, slots, columns), outs.dtype),
            dma((depth, lanes)), dma((depth, lanes)), dma((depth,)), dma((depth,)), dma((depth,)),
        ],
        compiler_params=pltpu.CompilerParams(
            collective_id=2, has_side_effects=True, vmem_limit_bytes=48 * 1024 * 1024),
        name="return_rows",
    )(outs, metas)


def earlier_same(ids):
    order = jnp.arange(ids.shape[0], dtype=jnp.int32)
    same = (ids[:, None] == ids[None, :]) & (order[None, :] < order[:, None])
    return jnp.sum(same.astype(jnp.int32), axis=1)


def on_device(
    dims,
    queries_small,
    queries_large,
    kv_small,
    kv_large,
    cum_small,
    cum_large,
    residual,
    out_small,
    out_large,
    gain_mix,
    gain_route,
    gain_blend,
    w_gate,
    w_up,
    w_down,
    route,
    route_bias,
):
    tokens_here = queries_small.shape[0]
    heads_small = cum_small.shape[0]
    heads_large = cum_large.shape[0]
    size_small = kv_small.shape[1] // 2
    size_large = kv_large.shape[1] // 2
    kv_all, cum_all = gather_keys(
        dims,
        jnp.concatenate([kv_small, kv_large], axis=1),
        jnp.concatenate([cum_small, cum_large], axis=0),
    )
    group = math.gcd(dims[1] * dims[2], 4)
    attn_small, attn_large = attend(
        queries_small,
        queries_large,
        kv_all,
        cum_all,
        (heads_small, heads_large, size_small, size_large),
        group,
    )
    row_count = tokens_here // lax.axis_size("tp")
    whole_small, whole_large = (
        lax.all_to_all(attn_small, "tp", split_axis=0, concat_axis=1, tiled=True),
        lax.all_to_all(attn_large, "tp", split_axis=0, concat_axis=1, tiled=True),
    )
    mixer_out = jnp.dot(whole_small, out_small, preferred_element_type=jnp.float32) + jnp.dot(
        whole_large, out_large, preferred_element_type=jnp.float32
    )
    mixed = (residual.astype(jnp.float32) + rms_scale(mixer_out, gain_mix)).astype(jnp.bfloat16)
    routed = rms_scale(mixed.astype(jnp.float32), gain_route).astype(jnp.bfloat16)
    experts = lax.axis_size(("sp", "tp"))
    cores = lax.axis_size("tp")
    depth = dims[0]
    lanes = experts // depth
    capacity = 4 * row_count // experts
    slots = capacity * lanes // 2
    group_ids = route[0] // lanes
    row_slots = group_ids * slots + earlier_same(group_ids)
    row_table = row_slots[None, :] == jnp.arange(depth * slots, dtype=jnp.int32)[:, None]
    flat_ids = route.reshape(2 * row_count)
    places = (flat_ids % lanes * capacity + earlier_same(flat_ids) + 1).astype(jnp.float32)
    facts = jnp.stack(
        [places[:row_count], places[row_count:], jax.nn.sigmoid(route_bias), jax.nn.sigmoid(-route_bias)]
    )
    meta = jnp.sum(jnp.where(row_table[None], facts[:, None, :], 0.0), axis=2)
    meta = meta.reshape(4, depth, slots).transpose(1, 0, 2)
    meta = jnp.pad(meta, ((0, 0), (0, 4), (0, -slots % 128)))
    outgoing = jnp.dot(
        row_table.astype(jnp.bfloat16), routed, preferred_element_type=jnp.float32
    ).astype(jnp.bfloat16)
    received, metas = dispatch(
        outgoing.reshape(depth, slots, routed.shape[1]), meta, lanes, cores, capacity
    )
    row_total = received.shape[0] * received.shape[1]
    expert_rows = received.reshape(row_total, received.shape[2])
    gate_pre = jnp.dot(expert_rows, w_gate[0], preferred_element_type=jnp.float32)
    up_pre = jnp.dot(expert_rows, w_up[0], preferred_element_type=jnp.float32)
    hidden = (jax.nn.silu(gate_pre) * up_pre).astype(jnp.bfloat16)
    expert_out = jnp.dot(hidden, w_down[0], preferred_element_type=jnp.float32).astype(jnp.bfloat16)
    returned = give_back(expert_out.reshape(received.shape), metas, lanes, cores, slots)
    blended = lax.dot_general(
        row_table.astype(jnp.bfloat16),
        returned.reshape(depth * slots, routed.shape[1]),
        (((0,), (0,)), ((), ())),
        preferred_element_type=jnp.float32,
    )
    return (mixed.astype(jnp.float32) + rms_scale(blended, gain_blend)).astype(jnp.bfloat16)


def solution(mesh):
    in_specs = (
        P("sp", "tp"),
        P("sp", "tp"),
        P("sp", None),
        P("sp", None),
        P("tp", "sp"),
        P("tp", "sp"),
        P(("sp", "tp"), None),
        P(),
        P(),
        P(),
        P(),
        P(),
        P(("sp", "tp"), None, None),
        P(("sp", "tp"), None, None),
        P(("sp", "tp"), None, None),
        P(None, ("sp", "tp")),
        P(("sp", "tp")),
    )
    out_specs = P(("sp", "tp"), None)
    return jax.shard_map(
        functools.partial(on_device, mesh_shape(mesh)), mesh=mesh, in_specs=in_specs, out_specs=out_specs, check_vma=False
    )
```
